32 devices in a mesh: gr: 2 (over x), sp: 8 (over z, y), tp: 2 (over core).
Axes of the slice: x: 2, y: 2, z: 4, core: 2. Of those that a mesh axis runs over, the one named last changes fastest.
Arguments:
- inputs: bfloat16 [4096, 2048], P(('gr', 'sp'), 'tp'), parts along dimension 0, may hold values from -6 to 6
- x_weight: bfloat16 [2048, 4096], P(None, 'tp'), may hold values from -0.125 to 0.125
- b_weight: bfloat16 [2048, 2048], P(None, 'tp'), may hold values from -0.125 to 0.125
- dt_weight: bfloat16 [2048, 128], replicated, may hold values from -0.125 to 0.125
- dt_bias: float32 [2, 64], replicated, may hold values from -2 to -1
- decay_rate: float32 [2, 64], replicated, may hold values from 0.3 to 10
- conv_x: bfloat16 [5, 4096], P(None, 'tp'), may hold values from -2.5 to 2.5
- conv_b: bfloat16 [5, 2048], P(None, 'tp'), may hold values from -2.5 to 2.5
- query_c: bfloat16 [2, 16, 128], P('gr', 'tp'), parts along dimension 0, may hold values from -6 to 6
- query_gate: bfloat16 [2, 64, 64], P('gr', 'tp'), parts along dimension 0, may hold values from -6 to 6
- read_span: int32 [2], P('gr'), parts along dimension 0, may hold values from 0 to 15
- read_gain: float32 [64, 64], P('tp'), may hold values from 0.1 to 1.9
Outputs:
- span_cache: bfloat16 [32, 2, 64, 8192], P('gr', None, 'tp', 'sp'), parts along dimension 0
- first_read: bfloat16 [2, 64, 64], P('gr', 'tp'), parts along dimension 0
The draws below stay inside these ranges and needn't reach their ends.
There are 2 independent parts, one for each index of `gr`. The reference program is written for one: setup_inputs(seed, part) draws one part's arguments, and reference() takes and returns one part's arrays. A program takes and returns all parts, laid end to end along the dimension named above; an argument that names none is the same for every part. Nothing has to cross between parts.
Inputs may be any that keep to these rules, and one draw needn't show every extreme that they name: read_span holds one span index from 0 to 15.
All inputs are finite; a program needn't handle non-finite values.
Results may differ from the reference program's by a relative error of at most 0.009.
Values may be sent and summed in bfloat16 or wider, within the bound.
A program may use at most 64 MiB of HBM per device.

```python
import math
import jax
import jax.numpy as jnp
from jax import lax

D = 2048
H = 64
P_SIZE = 64
G = 16
N = 128
KW = 5
SPAN = 128
LEN = 2048
SPANS = 16


def levels(rng, extent, shards, least, high):
    def one(dim, parts):
        heights = jax.random.uniform(jax.random.fold_in(jax.random.fold_in(rng, 6), dim), (parts,), jnp.float32, least / len(shards), high / len(shards))
        return jnp.repeat(jnp.exp(heights), extent[dim] // parts).reshape((-1,) + (1,) * (len(extent) - dim - 1))

    level = one(*shards[0])
    for cut in shards[1:]:
        level = level * one(*cut)
    return level


def gaussian(rng, extent, width, limit, split=(), kind=jnp.bfloat16):
    entries = jax.random.normal(rng, extent, jnp.float32) * width
    if len(split) > 0:
        entries = levels(rng, extent, split, -0.22, 0.18) * entries
    return jnp.clip(entries, min=-limit, max=limit).astype(kind)


def setup_inputs(seed: int = 0, part: int = 0) -> dict:
    arg_keys = jax.random.split(jax.random.key(seed), 13)
    part_keys = jax.random.split(jax.random.fold_in(arg_keys[12], part), 13)
    return {
        "inputs": gaussian(part_keys[0], (LEN, D), 1.0, 6.0, ((0, 8), (1, 2))),
        "x_weight": gaussian(arg_keys[1], (D, H * P_SIZE), D ** -0.5, 0.125, ((1, 2),)),
        "b_weight": gaussian(arg_keys[2], (D, G * N), D ** -0.5, 0.125, ((1, 2),)),
        "dt_weight": gaussian(arg_keys[3], (D, 2 * H), D ** -0.5, 0.125),
        "dt_bias": jnp.clip(jax.random.uniform(arg_keys[4], (2, H), jnp.float32, -2.0, -1.0), -2.0, -1.0),
        "decay_rate": jnp.clip(jnp.exp(jax.random.uniform(arg_keys[5], (2, H), jnp.float32, math.log(0.3), math.log(10.0))), 0.3, 10.0),
        "conv_x": gaussian(arg_keys[6], (KW, H * P_SIZE), KW ** -0.5, 2.5, ((1, 2),)),
        "conv_b": gaussian(arg_keys[7], (KW, G * N), KW ** -0.5, 2.5, ((1, 2),)),
        "query_c": gaussian(part_keys[8], (1, G, N), 1.0, 6.0, ((1, 2),)),
        "query_gate": gaussian(part_keys[9], (1, H, P_SIZE), 1.0, 6.0, ((1, 2),)),
        "read_span": jax.random.randint(part_keys[10], (1,), 0, SPANS).astype(jnp.int32),
        "read_gain": jnp.clip(1.0 + 0.18 * jax.random.normal(arg_keys[11], (H, P_SIZE), jnp.float32), 0.1, 1.9),
    }


EPSILON = 1e-06

def conv_silu(projected, taps):
    kernel = taps.shape[0]
    reach = kernel // 2
    length = projected.shape[0]
    padded = jnp.pad(projected.astype(jnp.float32), ((reach, reach), (0, 0)))
    result = jnp.zeros((length, projected.shape[1]), jnp.float32)
    for offset in range(kernel):
        result = result + taps[offset].astype(jnp.float32) * padded[offset:offset + length]
    return jax.nn.silu(result).astype(jnp.bfloat16)

def span_states(value_rows, key_rows, step_sizes, log_decay):
    running = jnp.cumsum(log_decay, axis=1)
    closing = running[:, -1]
    forward = jnp.exp(closing[:, None, 0] - running[:, :, 0]) * step_sizes[:, :, 0]
    backward = jnp.exp(running[:, :, 1] - log_decay[:, :, 1]) * step_sizes[:, :, 1]
    weights = jnp.stack([forward, backward], axis=2)
    states = jnp.einsum('kseh,kshn,kshp->kehnp', weights, key_rows.astype(jnp.float32), value_rows.astype(jnp.float32))
    return (states, closing)

def read_weights(span_logs, chosen):
    span_count = span_logs.shape[0]
    ahead_sum = jnp.cumsum(span_logs[:, 0], axis=0)
    behind = jnp.flip(jnp.cumsum(jnp.flip(span_logs[:, 1], 0), axis=0), 0)
    positions = jnp.arange(span_count, dtype=jnp.int32)[:, None]
    ahead_pick = lax.dynamic_slice_in_dim(ahead_sum, chosen, 1, 0)
    behind_pick = lax.dynamic_slice_in_dim(behind, chosen, 1, 0)
    before = positions <= chosen
    after = positions >= chosen
    forward = jnp.where(before, jnp.exp(jnp.where(before, ahead_pick - ahead_sum, 0.0)), 0.0)
    backward = jnp.where(after, jnp.exp(jnp.where(after, behind_pick - behind, 0.0)), 0.0)
    return jnp.stack([forward, backward], axis=1)

def reference(inputs, x_weight, b_weight, dt_weight, dt_bias, decay_rate, conv_x, conv_b, query_c, query_gate, read_span, read_gain):
    length = inputs.shape[0]
    values = conv_silu(jnp.dot(inputs, x_weight, preferred_element_type=jnp.float32).astype(jnp.bfloat16), conv_x)
    key_rows = conv_silu(jnp.dot(inputs, b_weight, preferred_element_type=jnp.float32).astype(jnp.bfloat16), conv_b)
    dt_raw = jnp.dot(inputs, dt_weight, preferred_element_type=jnp.float32).astype(jnp.bfloat16).reshape(length, 2, H)
    step_sizes = jax.nn.softplus(dt_raw.astype(jnp.float32) + dt_bias)
    log_decay = -(step_sizes * decay_rate) / length
    span_count = length // SPAN
    step_sizes = step_sizes.reshape(span_count, SPAN, 2, H)
    log_decay = log_decay.reshape(span_count, SPAN, 2, H)
    span_logs = lax.optimization_barrier(jnp.sum(log_decay, axis=1))
    weights = read_weights(span_logs, read_span[0])
    per_group = H // G

    def one_group(group_index):
        first_head = group_index * per_group
        group_values = lax.dynamic_slice_in_dim(values, first_head * P_SIZE, per_group * P_SIZE, 1).reshape(span_count, SPAN, per_group, P_SIZE)
        group_keys = lax.dynamic_slice_in_dim(key_rows, group_index * N, N, 1).reshape(span_count, SPAN, 1, N)
        group_keys = jnp.broadcast_to(group_keys, (span_count, SPAN, per_group, N))
        group_steps = lax.dynamic_slice_in_dim(step_sizes, first_head, per_group, 3)
        group_logs = lax.dynamic_slice_in_dim(log_decay, first_head, per_group, 3)
        states, unused = span_states(group_values, group_keys, group_steps, group_logs)
        row_block = states.reshape(span_count, 2, per_group, N * P_SIZE).astype(jnp.bfloat16)
        group_weights = lax.dynamic_slice_in_dim(weights, first_head, per_group, 2)
        gathered = jnp.einsum('jeh,jehx->hx', group_weights, row_block.astype(jnp.float32))
        return (row_block, gathered)
    row_block, gathered = lax.map(one_group, jnp.arange(G, dtype=jnp.int32))
    span_cache = jnp.transpose(row_block, (1, 2, 0, 3, 4)).reshape(span_count, 2, H, N * P_SIZE)
    read_state = gathered.reshape(H, N, P_SIZE)
    query_cols = jnp.repeat(query_c[0].astype(jnp.float32), per_group, axis=0)
    read_total = jnp.einsum('hnp,hn->hp', read_state, query_cols)
    gated_read = read_total * jax.nn.silu(query_gate[0].astype(jnp.float32))
    mean_square = jnp.mean(gated_read * gated_read)
    first_read = (gated_read * lax.rsqrt(mean_square + EPSILON) * read_gain)[None].astype(jnp.bfloat16)
    return (span_cache, first_read)
```

```python
import functools
import math

import jax
import jax.numpy as jnp
from jax import lax
from jax.experimental import pallas as pl
from jax.experimental.pallas import tpu as pltpu
from jax.sharding import PartitionSpec as P

H = 64
P_SIZE = 64
G = 16
N = 128
KW = 5
SPAN = 128
EPSILON = 1e-06
PER = H // G
LINE = 4
EDGE = 16
TILE = 8
LANES = 128
MESH = pl.DeviceIdType.MESH
F32 = jnp.float32
BF16 = jnp.bfloat16


def silu_of_half(h):
    return h + h * jnp.tanh(h)


def kernel(
    n, width, x, xw, bw, dtw_h, bias_h, rate_h, cx_h, cb_h, q_h, gate_h, chosen, gain_h,
    out, fr,
    bias, rate, cx, cb, q, gate, gain,
    xall, xwv, bwv, kw, kw2, p0, p1, pk, vs, kt, kt2, wt, held, stage,
    taps_x, taps_b, taps_k, taps_k2, tri, turn, offset, speed, q8, spread, logs, parts, total_rows, reads, squares,
    sem_small, sem_w, sem_own, sem_edge, sem_x, sem_in, sem_fwd, sem_hand, sem_c, sem_y, sem_sq,
    sem_out, sem_self, sem_round,
):
    s = lax.axis_index("sp")
    c = lax.axis_index("tp")
    tokens, feats = x.shape
    spans = tokens // SPAN
    heads = xw.shape[1] // P_SIZE
    groups = heads // PER
    ny = n // LINE
    z = s // ny
    y = lax.rem(s, ny)
    side = z // (LINE // 2)
    zz = z + side * (LINE - 1 - 2 * z)
    is_end = zz == 0
    is_mid = zz == 1
    blocks = heads // TILE
    bcols = TILE * P_SIZE
    share = N // LINE
    half = share // 2
    per_y = half // ny
    pitch = 2 * half + 4
    gb = min(PER, groups)
    kblocks = groups // gb
    kcols = kblocks * LANES
    rows = EDGE + tokens
    cut = SPAN + 2 * EDGE
    lane = lax.broadcasted_iota(jnp.int32, (1, LANES), 1)
    low = lane < P_SIZE
    span_cut = ((EDGE, cut - EDGE), (cut, rows - cut), (0, EDGE))

    def at_line(m):
        return m + side * (LINE - 1 - 2 * m)

    def mate(k):
        return lax.rem(c + k, width)

    def peer(k):
        return lax.rem(s + k, n)

    mine = pl.ds(pl.multiple_of(c * feats, feats), feats)

    smalls = [
        pltpu.make_async_copy(a, b, sem_small.at[i])
        for i, (a, b) in enumerate(
            (
                (bias_h, bias), (rate_h, rate), (cx_h, cx), (cb_h, cb),
                (q_h, q), (gate_h, gate), (gain_h, gain),
                (dtw_h, kw.at[:, pl.ds(kcols, 2 * H)]),
            )
        )
    ]
    own = pltpu.make_async_copy(x, xall.at[zz, pl.ds(EDGE, tokens), mine], sem_own)

    x_weight = pltpu.make_async_copy(xw, xwv, sem_w.at[0])
    b_weight = pltpu.make_async_copy(bw, bwv, sem_w.at[1])
    own.start()
    for copy in smalls:
        copy.start()
    b_weight.start()
    x_weight.start()

    @pl.when(s == 0)
    def _():
        xall[zz, pl.ds(8, 8), :] = jnp.zeros((8, xall.shape[2]), BF16)

    @pl.when(s == n - 1)
    def _():
        xall[zz, pl.ds(0, 8), :] = jnp.zeros((8, xall.shape[2]), BF16)

    barrier = pltpu.get_barrier_semaphore()
    def greet(sem):
        def tell(sp, tp):
            pl.semaphore_signal(
                sem, inc=1, device_id={"sp": sp, "tp": tp}, device_id_type=MESH
            )

        tell(at_line(1 - zz) * ny + y, c)

        @pl.when(is_mid)
        def _():
            tell(at_line(LINE // 2) * ny + y, c)

        for k in range(1, ny):
            tell(z * ny + lax.rem(y + k, ny), c)
        for k in range(1, width):
            tell(s, mate(k))

    def met(sem):
        pl.semaphore_wait(sem, zz + ny + width - 1)

    greet(barrier)
    met(barrier)

    def region(u, piece):
        start, size = span_cut[piece]
        return xall.at[u, pl.ds(start, size), mine]

    def source(piece):
        if piece == 2:
            return region(zz, 2)
        start, size = span_cut[piece]
        return x.at[pl.ds(start - EDGE, size), :]

    def edge(up):
        target = lax.rem(s + (1 if up else n - 1), n)
        tz = target // ny
        slot = tz + (tz // (LINE // 2)) * (LINE - 1 - 2 * tz)
        return pltpu.make_async_remote_copy(
            src_ref=x.at[pl.ds(tokens - 8 if up else 0, 8), :],
            dst_ref=xall.at[slot, pl.ds(8 if up else 0, 8), mine],
            send_sem=sem_edge.at[0, up],
            recv_sem=sem_edge.at[1, up],
            device_id={"sp": target, "tp": c},
            device_id_type=MESH,
        )

    def send_own(j, piece):
        goal = 1 - zz if j == 0 else LINE // 2
        slot = zz if j == 0 else LINE - 1 - zz
        return pltpu.make_async_remote_copy(
            src_ref=source(piece),
            dst_ref=region(slot, piece),
            send_sem=sem_x.at[j],
            recv_sem=sem_in.at[slot, piece % 2],
            device_id={"sp": at_line(goal) * ny + y, "tp": c},
            device_id_type=MESH,
        )

    def area(u, part, times=1):
        tall = (cut, rows - cut, rows)[part]
        return xall.at[u, pl.ds(0, tall), pl.ds(0, times * feats)]

    def arrived(u, part):
        at = area(u, part)
        return pltpu.make_async_remote_copy(
            src_ref=at,
            dst_ref=at,
            send_sem=sem_x.at[0],
            recv_sem=sem_in.at[u, part],
            device_id={"sp": at_line(1 - zz) * ny + y, "tp": c},
            device_id_type=MESH,
        )

    def left(sem, u, times=1):
        at = area(u, 2, times)
        return pltpu.make_async_copy(at, at, sem)

    def forward(piece):
        return pltpu.make_async_remote_copy(
            src_ref=region(2, piece),
            dst_ref=region(2, piece),
            send_sem=sem_fwd,
            recv_sem=sem_in.at[2, piece % 2],
            device_id={"sp": at_line(0) * ny + y, "tp": c},
            device_id_type=MESH,
        )

    def hand(u, piece, k, first=False):
        return pltpu.make_async_remote_copy(
            src_ref=source(piece) if first else region(u, piece),
            dst_ref=region(u, piece),
            send_sem=sem_hand.at[0, u, 0],
            recv_sem=sem_hand.at[1, u, piece % 2],
            device_id={"sp": s, "tp": mate(k)},
            device_id_type=MESH,
        )

    early, late, everything = (0, 2), (1,), (0, 2, 1)

    def parts_of(pieces):
        return [0] * (0 in pieces) + [1] * (1 in pieces)

    def take(u, pieces=everything):
        for part in parts_of(pieces):
            arrived(u, part).wait_recv()

    def pass_on(pieces):
        for piece in pieces:
            forward(piece).start()

    def hand_on(u, pieces=everything):
        for piece in pieces:
            for k in range(1, width):
                hand(u, piece, k).start()

    def handed(u, pieces=everything):
        for part in parts_of(pieces):
            at = area(u, part, width - 1)
            pltpu.make_async_copy(at, at, sem_hand.at[1, u, part]).wait()

    send_own(0, 0).start()

    @pl.when(is_mid)
    def _():
        send_own(1, 0).start()

    greet(sem_round.at[0])
    for piece in range(2):
        for k in range(1, width):
            hand(zz, piece, k, True).start()

    row2 = lax.broadcasted_iota(jnp.int32, (2 * SPAN, 2 * SPAN), 0)
    col2 = lax.broadcasted_iota(jnp.int32, (2 * SPAN, 2 * SPAN), 1)
    at_s = lax.rem(row2, SPAN)
    later = (col2 < SPAN) & (at_s > col2)
    earlier = (col2 >= SPAN) & (at_s < col2 - SPAN)
    tri[...] = jnp.where(later | earlier, 1.0, 0.0).astype(F32).astype(BF16)
    met(sem_round.at[0])
    greet(sem_round.at[1])

    @pl.when(s < n - 1)
    def _():
        edge(1).start()

    @pl.when(s > 0)
    def _():
        edge(0).start()


    for copy in smalls:
        copy.wait()

    heads_rows = pl.ds(pl.multiple_of(c * heads, heads), heads)
    heads_rows_back = pl.ds(pl.multiple_of(H + c * heads, heads), heads)

    def my_heads(value, slot):
        turn[slot] = jnp.transpose(value)
        return jnp.concatenate([turn[slot, heads_rows, :], turn[slot, heads_rows_back, :]], axis=0)

    wide = (LANES, 2 * H)
    offset[...] = my_heads(
        jnp.broadcast_to(jnp.concatenate([bias[0:1, :], bias[1:2, :]], axis=1), wide), 0
    )
    speed[...] = my_heads(
        jnp.broadcast_to(jnp.concatenate([rate[0:1, :], rate[1:2, :]], axis=1), wide), 1
    )
    taps_x[0:KW] = cx[...].astype(F32) * 0.5
    taps_b[0:KW] = cb[...].astype(F32) * 0.5
    q8[...] = jnp.zeros(q8.shape, F32)
    q8[0:groups] = q[0].astype(F32)

    def slice_weights():
        b_weight.wait()
        wide_in = gb * N
        pick_row = lax.broadcasted_iota(jnp.int32, (wide_in, 2 * LANES), 0)
        pick_col = lax.broadcasted_iota(jnp.int32, (wide_in, 2 * LANES), 1)
        base = jnp.where(pick_col < LANES, z * share, at_line(0) * share)
        inner = lax.rem(pick_col, LANES)
        wanted = (inner // share) * N + base + lax.rem(inner, share)
        pick = jnp.where((pick_row == wanted) & (inner < gb * share), 1.0, 0.0)
        pick = pick.astype(F32).astype(BF16)
        for j in range(kblocks):
            from_cols = pl.ds(j * wide_in, wide_in)
            to = pl.ds(j * LANES, LANES)
            tap = jnp.dot(cb[:, from_cols], pick, preferred_element_type=F32) * 0.5
            taps_k[0:KW, to] = tap[:, :LANES]
            taps_k2[0:KW, to] = tap[:, LANES:]
            step = 512

            @pl.loop(0, bwv.shape[0] // step)
            def _(i):
                at = pl.ds(pl.multiple_of(i * step, step), step)
                got = jnp.dot(bwv[at, from_cols], pick, preferred_element_type=F32).astype(BF16)
                kw[at, to] = got[:, :LANES]
                kw2[at, to] = got[:, LANES:]

    def weigh(k, raw):
        raw = my_heads(raw, k % 2).astype(BF16).astype(F32) + offset[...]
        step = jnp.maximum(raw, 0.0) + jnp.log1p(jnp.exp(-jnp.abs(raw)))
        decay = -(step * speed[...]) / (tokens * n)
        high = decay.astype(BF16)
        rest = (decay - high.astype(F32)).astype(BF16)
        both = jnp.dot(
            jnp.concatenate([high, rest], axis=1), tri[...], preferred_element_type=F32
        )
        first = lax.broadcasted_iota(jnp.int32, (2 * heads, LANES), 0) < heads
        wt[k] = jnp.exp(jnp.where(first, both[:, :SPAN], both[:, SPAN:])) * step
        return decay

    slice_weights()

    @pl.when(s > 0)
    def _():
        edge(1).wait_recv()

    @pl.when(s < n - 1)
    def _():
        edge(0).wait_recv()

    own.wait()
    send_own(0, 2).start()
    send_own(0, 1).start()

    @pl.when(is_mid)
    def _():
        send_own(1, 2).start()
        send_own(1, 1).start()

    for k in range(1, width):
        hand(zz, 2, k).start()

    met(sem_round.at[1])
    greet(sem_round.at[2])
    handed(zz)

    mine_raw = jnp.dot(
        xall[zz, pl.ds(EDGE, tokens), :], kw[:, kcols:], preferred_element_type=F32
    )
    closing = jnp.zeros((2 * heads, LANES), F32)
    for k in range(spans):
        decay = weigh(k, mine_raw[k * SPAN : (k + 1) * SPAN])
        closing = jnp.where(lane == k, jnp.sum(decay, axis=1, keepdims=True), closing)
    if 2 * heads < LANES:
        closing = jnp.concatenate([closing, jnp.zeros((LANES - 2 * heads, LANES), F32)], axis=0)
    logs[s] = jnp.transpose(closing)[0:8]

    def count(ref, times, sem):
        at = ref.at[pl.ds(0, times)]
        return pltpu.make_async_copy(at, at, sem)

    def log_copy(k):
        return pltpu.make_async_remote_copy(
            src_ref=logs.at[s],
            dst_ref=logs.at[s],
            send_sem=sem_c.at[0],
            recv_sem=sem_c.at[1],
            device_id={"sp": peer(k), "tp": c},
            device_id_type=MESH,
        )

    met(sem_round.at[2])

    @pl.loop(1, n)
    def _(k):
        log_copy(k).start()

    def around(u, k):
        if k is None:
            return xall[u]
        if k == 0:
            return xall[u, pl.ds(0, SPAN + 2 * EDGE), :]
        last = xall[u, pl.ds(k * SPAN, rows - k * SPAN), :]
        if k + 1 < spans:
            return last[0 : SPAN + 2 * EDGE]
        return jnp.concatenate([last, xall[u, pl.ds(0, EDGE), :]], axis=0)

    def put(p, value, wrap=True):
        tall = value.shape[0]
        for i in range(value.shape[1] // LANES):
            part = value[:, i * LANES : (i + 1) * LANES]
            p[i, pl.ds(0, tall), :] = part
            if wrap:
                p[i, pl.ds(tall, 8), :] = part[0:8]

    def mix(p, i, taps, col, start, size):
        mixed = None
        for k in range(KW):
            moved = p[i, pl.ds(EDGE + start + k - KW // 2, size), :]
            term = taps[k : k + 1, col : col + LANES] * moved
            mixed = term if mixed is None else mixed + term
        return silu_of_half(mixed)

    def keys_of(p, taps, target, only):
        for i in range(kblocks):
            for k in range(spans) if only is None else (only,):
                start = k * SPAN if only is None else 0
                mixed = mix(p, i, taps, i * LANES, start, SPAN)
                target[k, pl.ds(i * LANES, LANES), :] = jnp.transpose(mixed)

    def values_of(p, b, only):
        first = 0 if only is None else only * SPAN
        for i in range(bcols // LANES):
            col = b * bcols + i * LANES
            for r in range((tokens if only is None else SPAN) // 64):
                mixed = mix(p, i, taps_x, col, r * 64, 64)
                vs[pl.ds(first + r * 64, 64), col : col + LANES] = mixed.astype(BF16)

    def goal(u, k, b):
        span = (at_line(u) * ny + y) * spans + k
        return out.at[span, :, pl.ds(b * TILE, TILE), :]

    def state_copy(place, u, k, b, yk, line):
        place_sem = 1 if isinstance(line, int) else 0
        return pltpu.make_async_remote_copy(
            src_ref=stage.at[place, k, yk, b],
            dst_ref=goal(u, k, b),
            send_sem=sem_out.at[place_sem],
            recv_sem=sem_out.at[2],
            device_id={"sp": at_line(line) * ny + lax.rem(y + yk, ny), "tp": c},
            device_id_type=MESH,
        )

    def state_keep(u, k, b):
        return pltpu.make_async_copy(stage.at[u, k, 0, b], goal(u, k, b), sem_self)

    def states(place, keys, k, b):
        slot = (b * spans + k) % 2
        part = slice(k * SPAN, (k + 1) * SPAN)
        for pair in range(TILE // 2):
            h0 = b * TILE + pair * 2
            group = h0 // PER
            first = (group // gb) * LANES + (group % gb) * share
            even = keys[k, pl.ds(first, half, stride=2), :]
            odd = keys[k, pl.ds(first + 1, half, stride=2), :]
            scaled = []
            for h in range(2):
                for d in range(2):
                    weight = wt[k, pl.ds(d * heads + h0 + h, 1), :]
                    scaled.append(
                        jnp.concatenate([even * weight, odd * weight], axis=1).astype(BF16)
                    )
            col = h0 * P_SIZE
            v = vs[part, col : col + LANES].astype(F32)
            swapped = pltpu.roll(v, P_SIZE, 1)
            top = [jnp.where(low, v, 0.0), jnp.where(low, swapped, 0.0)]
            bottom = [jnp.where(low, 0.0, swapped), jnp.where(low, 0.0, v)]
            right = jnp.concatenate(
                [jnp.concatenate(top, axis=1), jnp.concatenate(bottom, axis=1)], axis=0
            ).astype(BF16)
            both = jnp.dot(
                jnp.concatenate(scaled, axis=0), right, preferred_element_type=F32
            )
            for h in range(2):
                held[slot, pl.ds((pair * 2 + h) * pitch, 2 * half), :] = both[
                    h * 2 * half : (h + 1) * 2 * half, h * LANES : (h + 1) * LANES
                ]
        for yk in range(ny):
            first = lax.rem(y + yk, ny) * per_y
            for d in range(2):
                for m in range(per_y):
                    piece = held[slot, pl.ds(d * half + first + m, TILE, stride=pitch), :]
                    stage[place, k, yk, b, d, :, m * LANES : (m + 1) * LANES] = piece.astype(BF16)

    def process(u, extra, only=None):
        wrap = only is None
        chosen_spans = range(spans) if only is None else (only,)
        both = jnp.dot(around(u, only), kw[...], preferred_element_type=F32)
        put(pk, both, wrap)
        if extra:
            put(p1, jnp.dot(around(u, only), kw2[...], preferred_element_type=F32), wrap)
        ps = (p0, p1)

        def values_dot(b):
            at = slice(b * bcols, (b + 1) * bcols)
            put(ps[b % 2], jnp.dot(around(u, only), xwv[:, at], preferred_element_type=F32), wrap)

        values_dot(0)
        keys_of(pk, taps_k, kt, only)
        if extra:
            keys_of(p1, taps_k2, kt2, only)
        for k in chosen_spans:
            start = k * SPAN if only is None else 0
            weigh(k, pk[kblocks, pl.ds(EDGE + start, SPAN), :])
        for b in range(blocks):
            if b + 1 < blocks:
                values_dot(b + 1)
            values_of(ps[b % 2], b, only)
            if extra:
                for k in chosen_spans:
                    states(LINE, kt2, k, b)
                    for yk in range(ny):
                        state_copy(LINE, u, k, b, yk, 0).start()
            for k in chosen_spans:
                states(u, kt, k, b)
                state_keep(u, k, b).start()
                for yk in range(1, ny):
                    state_copy(u, u, k, b, yk, zz).start()

    x_weight.wait()

    def part_copy(k):
        return pltpu.make_async_remote_copy(
            src_ref=parts.at[s],
            dst_ref=parts.at[s],
            send_sem=sem_y.at[0],
            recv_sem=sem_y.at[1],
            device_id={"sp": peer(k), "tp": c},
            device_id_type=MESH,
        )

    def own_read():
        seen = jnp.zeros((8, tokens), F32)
        which = lax.broadcasted_iota(jnp.int32, (8, LANES), 0)
        wide_in = gb * N
        for j in range(kblocks):
            at = slice(j * wide_in, (j + 1) * wide_in)
            put(p0, jnp.dot(xall[zz], bwv[:, at], preferred_element_type=F32))
            asked = []
            found = []
            for i in range(gb):
                asked.append(jnp.where(which == j * gb + i, q8[...], 0.0))
                found.append(mix(p0, i, taps_b, j * wide_in + i * LANES, 0, tokens).astype(BF16))
            seen = seen + lax.dot_general(
                jnp.concatenate(asked, axis=1).astype(BF16),
                jnp.concatenate(found, axis=1),
                (((1,), (1,)), ((), ())),
                preferred_element_type=F32,
            )

        head = lax.broadcasted_iota(jnp.int32, (heads, LANES), 0)
        line = lax.broadcasted_iota(jnp.int32, total_rows.shape, 0)
        for k in range(spans):
            part = slice(k * SPAN, (k + 1) * SPAN)
            for i in range(PER):
                spread[k, pl.ds(i, groups, stride=PER), :] = seen[0:groups, part]
            asked = jnp.concatenate([spread[k], spread[k]], axis=0)
            asked = (wt[k] * asked).astype(BF16)
            dense = [jnp.zeros(total_rows.shape, F32)] * 2
            for b in range(blocks):
                got = jnp.dot(
                    asked, vs[part, b * bcols : (b + 1) * bcols], preferred_element_type=F32
                )
                for i in range(bcols // LANES):
                    pair = b * (bcols // LANES) + i
                    mask = head == jnp.where(low, 2 * pair, 2 * pair + 1)
                    for d in range(2):
                        picked = got[d * heads : (d + 1) * heads, i * LANES : (i + 1) * LANES]
                        picked = jnp.sum(jnp.where(mask, picked, 0.0), axis=0, keepdims=True)
                        dense[d] = jnp.where(line == pair, picked, dense[d])
            for d in range(2):
                reads[k, d] = dense[d]

    def send_read():
        count(logs, n - 1, sem_c.at[1]).wait()

        every = logs[...]
        sub = lax.broadcasted_iota(jnp.int32, (8, LANES), 0)
        index = lax.broadcasted_iota(jnp.int32, every.shape, 0) * spans + lax.broadcasted_iota(
            jnp.int32, every.shape, 1
        )
        real = lax.broadcasted_iota(jnp.int32, every.shape, 1) < spans
        front = lane < heads
        r = chosen[0]
        table = jnp.zeros((8, LANES), F32)
        for k in range(spans):
            j = s * spans + k
            forward_on = real & (index > j) & (index <= r) & front[None]
            backward_on = real & (index < j) & (index >= r) & (~front)[None]
            total = jnp.sum(jnp.where(forward_on | backward_on, every, 0.0), axis=0)
            total = jnp.sum(total, axis=0, keepdims=True)
            ahead_on = jnp.where(j <= r, 1.0, 0.0)
            behind_on = jnp.where(j >= r, 1.0, 0.0)
            found = jnp.exp(total) * jnp.where(front, ahead_on, behind_on)
            table = jnp.where(sub == k, found, table)
        table = jnp.transpose(
            jnp.concatenate([table, jnp.zeros((LANES - 8, LANES), F32)], axis=0)
        )
        pairs = heads // 2
        dense = jnp.zeros((pairs, LANES), F32)
        for k in range(spans):
            for d in range(2):
                weight = jnp.broadcast_to(
                    table[d * heads : (d + 1) * heads, k : k + 1], (heads, LANES)
                )
                spread[d] = weight
                even = spread[d, pl.ds(0, pairs, stride=2), :]
                odd = spread[d, pl.ds(1, pairs, stride=2), :]
                dense = dense + jnp.where(low, even, odd) * reads[k, d, 0:pairs, :]
        parts[s, 0:pairs, :] = dense

        @pl.loop(1, n)
        def _(k):
            part_copy(k).start()

    def square(k):
        return pltpu.make_async_remote_copy(
            src_ref=squares.at[c],
            dst_ref=squares.at[c],
            send_sem=sem_sq.at[0],
            recv_sem=sem_sq.at[1],
            device_id={"sp": s, "tp": mate(k)},
            device_id_type=MESH,
        )

    def gather_read():
        count(parts, n - 1, sem_y.at[1]).wait()

        def add_part(i, total):
            return total + parts[i]

        total = lax.fori_loop(1, n, add_part, parts[0])[0 : heads // 2]
        spread[0, pl.ds(0, heads // 2, stride=2), :] = total
        spread[0, pl.ds(1, heads // 2, stride=2), :] = pltpu.roll(total, P_SIZE, 1)
        door = gate[0].astype(F32) * 0.5
        gated = spread[0][:, :P_SIZE] * silu_of_half(door)
        spread[1, :, 0:P_SIZE] = gated
        squares[c] = jnp.broadcast_to(jnp.sum(gated * gated, keepdims=True), (8, LANES))
        for k in range(1, width):
            square(k).start()

    def finish_read():
        count(squares, width - 1, sem_sq.at[1]).wait()
        mean = jnp.sum(squares[...], axis=0)[0:1, 0:1] / (H * P_SIZE)
        gated = spread[1, :, 0:P_SIZE]
        fr[0] = (gated * lax.rsqrt(mean + EPSILON) * gain[...]).astype(BF16)

    @pl.when(is_mid)
    def _():
        take(2, early)
        pass_on(early)

    @pl.loop(0, 3)
    def _(i):
        u = jnp.where(is_end, i, lax.rem(i + 1, 3))

        @pl.when(i > 0)
        def _():
            handed(u)

        process(u, False)

        @pl.when(i == 0)
        def _():
            @pl.when(is_end)
            def _():
                for piece in everything:
                    send_own(1, piece).start()
                take(1)
                hand_on(1)

            @pl.when(is_mid)
            def _():
                take(2, late)
                pass_on(late)
                hand_on(2)
                take(0)
                hand_on(0)

            own_read()

        @pl.when(i == 1)
        def _():
            send_read()

            @pl.when(is_end)
            def _():
                take(2)
                hand_on(2)

            @pl.when(is_mid)
            def _():
                take(3, early)
                hand_on(3, early)

    @pl.when(is_mid)
    def _():
        handed(3, early)
        process(3, True, 0)
        take(3, late)
        hand_on(3, late)
        handed(3, late)
        for k in range(1, spans):
            process(3, True, k)

    gather_read()
    finish_read()

    @pl.when(s < n - 1)
    def _():
        edge(1).wait_send()

    @pl.when(s > 0)
    def _():
        edge(0).wait_send()

    for j in range(2):
        left(sem_x.at[j], zz).wait()
    for u in range(3):
        left(sem_hand.at[0, u, 0], u, width - 1).wait()
    count(squares, width - 1, sem_sq.at[0]).wait()
    count(logs, n - 1, sem_c.at[0]).wait()
    count(parts, n - 1, sem_y.at[0]).wait()

    @pl.when(is_mid)
    def _():
        left(sem_fwd, 2).wait()
        left(sem_hand.at[0, 3, 0], 3, width - 1).wait()
        count(out, LINE * spans, sem_self).wait()
        count(out, LINE * (ny - 1) * spans, sem_out.at[0]).wait()
        count(out, ny * spans, sem_out.at[1]).wait()
        count(out, LINE * (ny - 1) * spans, sem_out.at[2]).wait()

    @pl.when(is_end)
    def _():
        count(out, (LINE - 1) * spans, sem_self).wait()
        count(out, (LINE - 1) * (ny - 1) * spans, sem_out.at[0]).wait()
        count(out, ((LINE - 1) * (ny - 1) + ny) * spans, sem_out.at[2]).wait()


def per_device(x, xw, bw, dtw, bias, rate, cx, cb, q, gate, chosen, gain):
    n = lax.axis_size("sp")
    width = lax.axis_size("tp")
    tokens, feats = x.shape
    depth = xw.shape[0]
    spans = tokens // SPAN
    heads = xw.shape[1] // P_SIZE
    groups = heads // PER
    blocks = heads // TILE
    columns = N * P_SIZE // n
    ny = n // LINE
    share = N // LINE
    gb = min(PER, groups)
    kblocks = groups // gb
    kcols = kblocks * LANES
    pblocks = TILE * P_SIZE // LANES
    tall = tokens + EDGE + 8
    small = (bias, rate, cx, cb, q, gate, gain)
    anywhere = pl.BlockSpec(memory_space=pl.ANY)
    vmem = pl.BlockSpec(memory_space=pltpu.VMEM)
    dma = pltpu.SemaphoreType.DMA
    return pl.pallas_call(
        functools.partial(kernel, n, width),
        out_shape=(
            pltpu.VMEM((spans * n, 2, heads, columns), BF16),
            pltpu.VMEM((1, heads, P_SIZE), BF16),
        ),
        in_specs=[anywhere] * 10 + [pl.BlockSpec(memory_space=pltpu.SMEM), anywhere],
        out_specs=(vmem, vmem),
        scratch_shapes=[pltpu.VMEM(a.shape, a.dtype) for a in small]
        + [
            pltpu.VMEM((LINE, tokens + EDGE, depth), BF16),
            pltpu.VMEM(xw.shape, BF16),
            pltpu.VMEM(bw.shape, BF16),
            pltpu.VMEM((depth, kcols + 2 * H), BF16),
            pltpu.VMEM((depth, kcols), BF16),
            pltpu.VMEM((pblocks, tall, LANES), F32),
            pltpu.VMEM((pblocks, tall, LANES), F32),
            pltpu.VMEM((kblocks + 1, tall, LANES), F32),
            pltpu.VMEM((tokens, heads * P_SIZE), BF16),
            pltpu.VMEM((spans, kcols, LANES), F32),
            pltpu.VMEM((spans, kcols, LANES), F32),
            pltpu.VMEM((spans, 2 * heads, LANES), F32),
            pltpu.VMEM((2, TILE * (share + 4) + share, LANES), F32),
            pltpu.VMEM((LINE + 1, spans, ny, blocks, 2, TILE, columns), BF16),
            pltpu.VMEM((8, cx.shape[1]), F32),
            pltpu.VMEM((8, cb.shape[1]), F32),
            pltpu.VMEM((8, kcols), F32),
            pltpu.VMEM((8, kcols), F32),
            pltpu.VMEM((2 * SPAN, 2 * SPAN), BF16),
            pltpu.VMEM((2, LANES, LANES), F32),
            pltpu.VMEM((2 * heads, LANES), F32),
            pltpu.VMEM((2 * heads, LANES), F32),
            pltpu.VMEM((8, N), F32),
            pltpu.VMEM((2, heads, LANES), F32),
            pltpu.VMEM((n, 8, LANES), F32),
            pltpu.VMEM((n, max(8, heads // 2), LANES), F32),
            pltpu.VMEM((max(8, heads // 2), LANES), F32),
            pltpu.VMEM((spans, 2, max(8, heads // 2), LANES), F32),
            pltpu.VMEM((width, 8, LANES), F32),
            dma((8,)),
            dma((2,)),
            dma,
            dma((2, 2)),
            dma((2,)),
            dma((LINE, 2)),
            dma,
            dma((2, LINE, 2)),
            dma((2,)),
            dma((2,)),
            dma((2,)),
            dma((3,)),
            dma,
            pltpu.SemaphoreType.REGULAR((3,)),
        ],
        compiler_params=pltpu.CompilerParams(
            collective_id=0, has_side_effects=True, vmem_limit_bytes=56 * 1024 * 1024
        ),
    )(x, xw, bw, dtw, bias, rate, cx, cb, q, gate, chosen, gain)


def solution(mesh):
    return jax.shard_map(
        per_device,
        mesh=mesh,
        in_specs=(
            P(("gr", "sp"), "tp"),
            P(None, "tp"),
            P(None, "tp"),
            P(),
            P(),
            P(),
            P(None, "tp"),
            P(None, "tp"),
            P("gr", "tp", None),
            P("gr", "tp", None),
            P("gr"),
            P("tp", None),
        ),
        out_specs=(P("gr", None, "tp", "sp"), P("gr", "tp", None)),
        check_vma=False,
    )
```

```python
import functools
import math

import jax
import jax.numpy as jnp
from jax import lax
from jax.experimental import pallas as pl
from jax.experimental.pallas import tpu as pltpu
from jax.sharding import PartitionSpec as P

H = 64
P_SIZE = 64
G = 16
N = 128
KW = 5
SPAN = 128
EPSILON = 1e-06
PER = H // G
LINE = 4
EDGE = 16
TILE = 8
LANES = 128
MESH = pl.DeviceIdType.MESH
F32 = jnp.float32
BF16 = jnp.bfloat16


def silu_of_half(h):
    return h + h * jnp.tanh(h)


def kernel(
    n, width, x, xw, bw, dtw_h, bias_h, rate_h, cx_h, cb_h, q_h, gate_h, chosen, gain_h,
    out, fr,
    bias, rate, cx, cb, q, gate, gain,
    xall, xwv, bwv, kw, kw2, p0, p1, pk, vs, kt, kt2, wt, held, stage,
    taps_x, taps_b, taps_k, taps_k2, tri, turn, offset, speed, q8, spread, logs, parts, total_rows, reads, squares,
    sem_small, sem_w, sem_own, sem_edge, sem_x, sem_in, sem_fwd, sem_hand, sem_c, sem_y, sem_sq,
    sem_out, sem_self, sem_round,
):
    s = lax.axis_index("sp")
    c = lax.axis_index("tp")
    tokens, feats = x.shape
    spans = tokens // SPAN
    heads = xw.shape[1] // P_SIZE
    groups = heads // PER
    ny = n // LINE
    z = s // ny
    y = lax.rem(s, ny)
    side = z // (LINE // 2)
    zz = z + side * (LINE - 1 - 2 * z)
    is_end = zz == 0
    is_mid = zz == 1
    blocks = heads // TILE
    bcols = TILE * P_SIZE
    share = N // LINE
    half = share // 2
    per_y = half // ny
    pitch = 2 * half + 4
    gb = min(PER, groups)
    kblocks = groups // gb
    kcols = kblocks * LANES
    rows = EDGE + tokens
    cut = SPAN + 2 * EDGE
    lane = lax.broadcasted_iota(jnp.int32, (1, LANES), 1)
    low = lane < P_SIZE
    span_cut = ((EDGE, cut - EDGE), (cut, rows - cut), (0, EDGE))

    def at_line(m):
        return m + side * (LINE - 1 - 2 * m)

    def mate(k):
        return lax.rem(c + k, width)

    def peer(k):
        return lax.rem(s + k, n)

    mine = pl.ds(pl.multiple_of(c * feats, feats), feats)

    smalls = [
        pltpu.make_async_copy(a, b, sem_small.at[i])
        for i, (a, b) in enumerate(
            (
                (bias_h, bias), (rate_h, rate), (cx_h, cx), (cb_h, cb),
                (q_h, q), (gate_h, gate), (gain_h, gain),
                (dtw_h, kw.at[:, pl.ds(kcols, 2 * H)]),
            )
        )
    ]
    own = pltpu.make_async_copy(x, xall.at[zz, pl.ds(EDGE, tokens), mine], sem_own)

    x_weight = pltpu.make_async_copy(xw, xwv, sem_w.at[0])
    b_weight = pltpu.make_async_copy(bw, bwv, sem_w.at[1])
    own.start()
    for copy in smalls:
        copy.start()
    b_weight.start()
    x_weight.start()

    @pl.when(s == 0)
    def _():
        xall[zz, pl.ds(8, 8), :] = jnp.zeros((8, xall.shape[2]), BF16)

    @pl.when(s == n - 1)
    def _():
        xall[zz, pl.ds(0, 8), :] = jnp.zeros((8, xall.shape[2]), BF16)

    barrier = pltpu.get_barrier_semaphore()
    def greet(sem):
        def tell(sp, tp):
            pl.semaphore_signal(
                sem, inc=1, device_id={"sp": sp, "tp": tp}, device_id_type=MESH
            )

        tell(at_line(1 - zz) * ny + y, c)

        @pl.when(is_mid)
        def _():
            tell(at_line(LINE // 2) * ny + y, c)

        for k in range(1, ny):
            tell(z * ny + lax.rem(y + k, ny), c)
        for k in range(1, width):
            tell(s, mate(k))

    def met(sem):
        pl.semaphore_wait(sem, zz + ny + width - 1)

    greet(barrier)
    met(barrier)

    def region(u, piece):
        start, size = span_cut[piece]
        return xall.at[u, pl.ds(start, size), mine]

    def source(piece):
        if piece == 2:
            return region(zz, 2)
        start, size = span_cut[piece]
        return x.at[pl.ds(start - EDGE, size), :]

    def edge(up):
        target = lax.rem(s + (1 if up else n - 1), n)
        tz = target // ny
        slot = tz + (tz // (LINE // 2)) * (LINE - 1 - 2 * tz)
        return pltpu.make_async_remote_copy(
            src_ref=x.at[pl.ds(tokens - 8 if up else 0, 8), :],
            dst_ref=xall.at[slot, pl.ds(8 if up else 0, 8), mine],
            send_sem=sem_edge.at[0, up],
            recv_sem=sem_edge.at[1, up],
            device_id={"sp": target, "tp": c},
            device_id_type=MESH,
        )

    def send_own(j, piece):
        goal = 1 - zz if j == 0 else LINE // 2
        slot = zz if j == 0 else LINE - 1 - zz
        return pltpu.make_async_remote_copy(
            src_ref=source(piece),
            dst_ref=region(slot, piece),
            send_sem=sem_x.at[j],
            recv_sem=sem_in.at[slot, piece % 2],
            device_id={"sp": at_line(goal) * ny + y, "tp": c},
            device_id_type=MESH,
        )

    def area(u, part, times=1):
        tall = (cut, rows - cut, rows)[part]
        return xall.at[u, pl.ds(0, tall), pl.ds(0, times * feats)]

    def arrived(u, part):
        at = area(u, part)
        return pltpu.make_async_remote_copy(
            src_ref=at,
            dst_ref=at,
            send_sem=sem_x.at[0],
            recv_sem=sem_in.at[u, part],
            device_id={"sp": at_line(1 - zz) * ny + y, "tp": c},
            device_id_type=MESH,
        )

    def left(sem, u, times=1):
        at = area(u, 2, times)
        return pltpu.make_async_copy(at, at, sem)

    def forward(piece):
        return pltpu.make_async_remote_copy(
            src_ref=region(2, piece),
            dst_ref=region(2, piece),
            send_sem=sem_fwd,
            recv_sem=sem_in.at[2, piece % 2],
            device_id={"sp": at_line(0) * ny + y, "tp": c},
            device_id_type=MESH,
        )

    def hand(u, piece, k, first=False):
        return pltpu.make_async_remote_copy(
            src_ref=source(piece) if first else region(u, piece),
            dst_ref=region(u, piece),
            send_sem=sem_hand.at[0, u, 0],
            recv_sem=sem_hand.at[1, u, piece % 2],
            device_id={"sp": s, "tp": mate(k)},
            device_id_type=MESH,
        )

    early, late, everything = (0, 2), (1,), (0, 2, 1)

    def parts_of(pieces):
        return [0] * (0 in pieces) + [1] * (1 in pieces)

    def take(u, pieces=everything):
        for part in parts_of(pieces):
            arrived(u, part).wait_recv()

    def pass_on(pieces):
        for piece in pieces:
            forward(piece).start()

    def hand_on(u, pieces=everything):
        for piece in pieces:
            for k in range(1, width):
                hand(u, piece, k).start()

    def handed(u, pieces=everything):
        for part in parts_of(pieces):
            at = area(u, part, width - 1)
            pltpu.make_async_copy(at, at, sem_hand.at[1, u, part]).wait()

    send_own(0, 0).start()

    @pl.when(is_mid)
    def _():
        send_own(1, 0).start()

    greet(sem_round.at[0])
    for piece in range(2):
        for k in range(1, width):
            hand(zz, piece, k, True).start()

    row2 = lax.broadcasted_iota(jnp.int32, (2 * SPAN, 2 * SPAN), 0)
    col2 = lax.broadcasted_iota(jnp.int32, (2 * SPAN, 2 * SPAN), 1)
    at_s = lax.rem(row2, SPAN)
    later = (col2 < SPAN) & (at_s > col2)
    earlier = (col2 >= SPAN) & (at_s < col2 - SPAN)
    tri[...] = jnp.where(later | earlier, 1.0, 0.0).astype(F32).astype(BF16)
    met(sem_round.at[0])
    greet(sem_round.at[1])

    @pl.when(s < n - 1)
    def _():
        edge(1).start()

    @pl.when(s > 0)
    def _():
        edge(0).start()


    for copy in smalls:
        copy.wait()

    heads_rows = pl.ds(pl.multiple_of(c * heads, heads), heads)
    heads_rows_back = pl.ds(pl.multiple_of(H + c * heads, heads), heads)

    def my_heads(value, slot):
        turn[slot] = jnp.transpose(value)
        return jnp.concatenate([turn[slot, heads_rows, :], turn[slot, heads_rows_back, :]], axis=0)

    wide = (LANES, 2 * H)
    offset[...] = my_heads(
        jnp.broadcast_to(jnp.concatenate([bias[0:1, :], bias[1:2, :]], axis=1), wide), 0
    )
    speed[...] = my_heads(
        jnp.broadcast_to(jnp.concatenate([rate[0:1, :], rate[1:2, :]], axis=1), wide), 1
    )
    taps_x[0:KW] = cx[...].astype(F32) * 0.5
    taps_b[0:KW] = cb[...].astype(F32) * 0.5
    q8[...] = jnp.zeros(q8.shape, F32)
    q8[0:groups] = q[0].astype(F32)

    def slice_weights():
        b_weight.wait()
        wide_in = gb * N
        pick_row = lax.broadcasted_iota(jnp.int32, (wide_in, 2 * LANES), 0)
        pick_col = lax.broadcasted_iota(jnp.int32, (wide_in, 2 * LANES), 1)
        base = jnp.where(pick_col < LANES, z * share, at_line(0) * share)
        inner = lax.rem(pick_col, LANES)
        wanted = (inner // share) * N + base + lax.rem(inner, share)
        pick = jnp.where((pick_row == wanted) & (inner < gb * share), 1.0, 0.0)
        pick = pick.astype(F32).astype(BF16)
        for j in range(kblocks):
            from_cols = pl.ds(j * wide_in, wide_in)
            to = pl.ds(j * LANES, LANES)
            tap = jnp.dot(cb[:, from_cols], pick, preferred_element_type=F32) * 0.5
            taps_k[0:KW, to] = tap[:, :LANES]
            taps_k2[0:KW, to] = tap[:, LANES:]
            step = 512

            @pl.loop(0, bwv.shape[0] // step)
            def _(i):
                at = pl.ds(pl.multiple_of(i * step, step), step)
                got = jnp.dot(bwv[at, from_cols], pick, preferred_element_type=F32).astype(BF16)
                kw[at, to] = got[:, :LANES]
                kw2[at, to] = got[:, LANES:]

    def weigh(k, raw):
        raw = my_heads(raw, k % 2).astype(BF16).astype(F32) + offset[...]
        step = jnp.maximum(raw, 0.0) + jnp.log1p(jnp.exp(-jnp.abs(raw)))
        decay = -(step * speed[...]) / (tokens * n)
        high = decay.astype(BF16)
        rest = (decay - high.astype(F32)).astype(BF16)
        both = jnp.dot(
            jnp.concatenate([high, rest], axis=1), tri[...], preferred_element_type=F32
        )
        first = lax.broadcasted_iota(jnp.int32, (2 * heads, LANES), 0) < heads
        wt[k] = jnp.exp(jnp.where(first, both[:, :SPAN], both[:, SPAN:])) * step
        return decay

    slice_weights()

    @pl.when(s > 0)
    def _():
        edge(1).wait_recv()

    @pl.when(s < n - 1)
    def _():
        edge(0).wait_recv()

    own.wait()
    send_own(0, 2).start()
    send_own(0, 1).start()

    @pl.when(is_mid)
    def _():
        send_own(1, 2).start()
        send_own(1, 1).start()

    for k in range(1, width):
        hand(zz, 2, k).start()

    met(sem_round.at[1])
    greet(sem_round.at[2])
    handed(zz)

    mine_raw = jnp.dot(
        xall[zz, pl.ds(EDGE, tokens), :], kw[:, kcols:], preferred_element_type=F32
    )
    closing = jnp.zeros((2 * heads, LANES), F32)
    for k in range(spans):
        decay = weigh(k, mine_raw[k * SPAN : (k + 1) * SPAN])
        closing = jnp.where(lane == k, jnp.sum(decay, axis=1, keepdims=True), closing)
    if 2 * heads < LANES:
        closing = jnp.concatenate([closing, jnp.zeros((LANES - 2 * heads, LANES), F32)], axis=0)
    logs[s] = jnp.transpose(closing)[0:8]

    def count(ref, times, sem):
        at = ref.at[pl.ds(0, times)]
        return pltpu.make_async_copy(at, at, sem)

    def log_copy(k):
        return pltpu.make_async_remote_copy(
            src_ref=logs.at[s],
            dst_ref=logs.at[s],
            send_sem=sem_c.at[0],
            recv_sem=sem_c.at[1],
            device_id={"sp": peer(k), "tp": c},
            device_id_type=MESH,
        )

    met(sem_round.at[2])

    @pl.loop(1, n)
    def _(k):
        log_copy(k).start()

    def around(u, k):
        if k is None:
            return xall[u]
        if k == 0:
            return xall[u, pl.ds(0, SPAN + 2 * EDGE), :]
        last = xall[u, pl.ds(k * SPAN, rows - k * SPAN), :]
        if k + 1 < spans:
            return last[0 : SPAN + 2 * EDGE]
        return jnp.concatenate([last, xall[u, pl.ds(0, EDGE), :]], axis=0)

    def put(p, value, wrap=True):
        tall = value.shape[0]
        for i in range(value.shape[1] // LANES):
            part = value[:, i * LANES : (i + 1) * LANES]
            p[i, pl.ds(0, tall), :] = part
            if wrap:
                p[i, pl.ds(tall, 8), :] = part[0:8]

    def mix(p, i, taps, col, start, size):
        mixed = None
        for k in range(KW):
            moved = p[i, pl.ds(EDGE + start + k - KW // 2, size), :]
            term = taps[k : k + 1, col : col + LANES] * moved
            mixed = term if mixed is None else mixed + term
        return silu_of_half(mixed)

    def keys_of(p, taps, target, only):
        for i in range(kblocks):
            for k in range(spans) if only is None else (only,):
                start = k * SPAN if only is None else 0
                mixed = mix(p, i, taps, i * LANES, start, SPAN)
                target[k, pl.ds(i * LANES, LANES), :] = jnp.transpose(mixed)

    def values_of(p, b, only):
        first = 0 if only is None else only * SPAN
        for i in range(bcols // LANES):
            col = b * bcols + i * LANES
            for r in range((tokens if only is None else SPAN) // 64):
                mixed = mix(p, i, taps_x, col, r * 64, 64)
                vs[pl.ds(first + r * 64, 64), col : col + LANES] = mixed.astype(BF16)

    def goal(u, k, b):
        span = (at_line(u) * ny + y) * spans + k
        return out.at[span, :, pl.ds(b * TILE, TILE), :]

    def state_copy(place, u, k, b, yk, line):
        place_sem = 1 if isinstance(line, int) else 0
        return pltpu.make_async_remote_copy(
            src_ref=stage.at[place, k, yk, b],
            dst_ref=goal(u, k, b),
            send_sem=sem_out.at[place_sem],
            recv_sem=sem_out.at[2],
            device_id={"sp": at_line(line) * ny + lax.rem(y + yk, ny), "tp": c},
            device_id_type=MESH,
        )

    def state_keep(u, k, b):
        return pltpu.make_async_copy(stage.at[u, k, 0, b], goal(u, k, b), sem_self)

    def states(place, keys, k, b):
        slot = (b * spans + k) % 2
        part = slice(k * SPAN, (k + 1) * SPAN)
        for pair in range(TILE // 2):
            h0 = b * TILE + pair * 2
            group = h0 // PER
            first = (group // gb) * LANES + (group % gb) * share
            even = keys[k, pl.ds(first, half, stride=2), :]
            odd = keys[k, pl.ds(first + 1, half, stride=2), :]
            scaled = []
            for h in range(2):
                for d in range(2):
                    weight = wt[k, pl.ds(d * heads + h0 + h, 1), :]
                    scaled.append(
                        jnp.concatenate([even * weight, odd * weight], axis=1).astype(BF16)
                    )
            col = h0 * P_SIZE
            v = vs[part, col : col + LANES].astype(F32)
            swapped = pltpu.roll(v, P_SIZE, 1)
            top = [jnp.where(low, v, 0.0), jnp.where(low, swapped, 0.0)]
            bottom = [jnp.where(low, 0.0, swapped), jnp.where(low, 0.0, v)]
            right = jnp.concatenate(
                [jnp.concatenate(top, axis=1), jnp.concatenate(bottom, axis=1)], axis=0
            ).astype(BF16)
            both = jnp.dot(
                jnp.concatenate(scaled, axis=0), right, preferred_element_type=F32
            )
            for h in range(2):
                held[slot, pl.ds((pair * 2 + h) * pitch, 2 * half), :] = both[
                    h * 2 * half : (h + 1) * 2 * half, h * LANES : (h + 1) * LANES
                ]
        for yk in range(ny):
            first = lax.rem(y + yk, ny) * per_y
            for d in range(2):
                for m in range(per_y):
                    piece = held[slot, pl.ds(d * half + first + m, TILE, stride=pitch), :]
                    stage[place, k, yk, b, d, :, m * LANES : (m + 1) * LANES] = piece.astype(BF16)

    def process(u, extra, only=None):
        wrap = only is None
        chosen_spans = range(spans) if only is None else (only,)
        both = jnp.dot(around(u, only), kw[...], preferred_element_type=F32)
        put(pk, both, wrap)
        if extra:
            put(p1, jnp.dot(around(u, only), kw2[...], preferred_element_type=F32), wrap)
        ps = (p0, p1)

        def values_dot(b):
            at = slice(b * bcols, (b + 1) * bcols)
            put(ps[b % 2], jnp.dot(around(u, only), xwv[:, at], preferred_element_type=F32), wrap)

        values_dot(0)
        keys_of(pk, taps_k, kt, only)
        if extra:
            keys_of(p1, taps_k2, kt2, only)
        for k in chosen_spans:
            start = k * SPAN if only is None else 0
            weigh(k, pk[kblocks, pl.ds(EDGE + start, SPAN), :])
        for b in range(blocks):
            if b + 1 < blocks:
                values_dot(b + 1)
            values_of(ps[b % 2], b, only)
            if extra:
                for k in chosen_spans:
                    states(LINE, kt2, k, b)
                    for yk in range(ny):
                        state_copy(LINE, u, k, b, yk, 0).start()
            for k in chosen_spans:
                states(u, kt, k, b)
                state_keep(u, k, b).start()
                for yk in range(1, ny):
                    state_copy(u, u, k, b, yk, zz).start()

    x_weight.wait()

    def part_copy(k):
        return pltpu.make_async_remote_copy(
            src_ref=parts.at[s],
            dst_ref=parts.at[s],
            send_sem=sem_y.at[0],
            recv_sem=sem_y.at[1],
            device_id={"sp": peer(k), "tp": c},
            device_id_type=MESH,
        )

    def own_read():
        seen = jnp.zeros((8, tokens), F32)
        which = lax.broadcasted_iota(jnp.int32, (8, LANES), 0)
        wide_in = gb * N
        for j in range(kblocks):
            at = slice(j * wide_in, (j + 1) * wide_in)
            put(p0, jnp.dot(xall[zz], bwv[:, at], preferred_element_type=F32))
            asked = []
            found = []
            for i in range(gb):
                asked.append(jnp.where(which == j * gb + i, q8[...], 0.0))
                found.append(mix(p0, i, taps_b, j * wide_in + i * LANES, 0, tokens).astype(BF16))
            seen = seen + lax.dot_general(
                jnp.concatenate(asked, axis=1).astype(BF16),
                jnp.concatenate(found, axis=1),
                (((1,), (1,)), ((), ())),
                preferred_element_type=F32,
            )

        head = lax.broadcasted_iota(jnp.int32, (heads, LANES), 0)
        line = lax.broadcasted_iota(jnp.int32, total_rows.shape, 0)
        for k in range(spans):
            part = slice(k * SPAN, (k + 1) * SPAN)
            for i in range(PER):
                spread[k, pl.ds(i, groups, stride=PER), :] = seen[0:groups, part]
            asked = jnp.concatenate([spread[k], spread[k]], axis=0)
            asked = (wt[k] * asked).astype(BF16)
            dense = [jnp.zeros(total_rows.shape, F32)] * 2
            for b in range(blocks):
                got = jnp.dot(
                    asked, vs[part, b * bcols : (b + 1) * bcols], preferred_element_type=F32
                )
                for i in range(bcols // LANES):
                    pair = b * (bcols // LANES) + i
                    mask = head == jnp.where(low, 2 * pair, 2 * pair + 1)
                    for d in range(2):
                        picked = got[d * heads : (d + 1) * heads, i * LANES : (i + 1) * LANES]
                        picked = jnp.sum(jnp.where(mask, picked, 0.0), axis=0, keepdims=True)
                        dense[d] = jnp.where(line == pair, picked, dense[d])
            for d in range(2):
                reads[k, d] = dense[d]

    def send_read():
        count(logs, n - 1, sem_c.at[1]).wait()

        every = logs[...]
        sub = lax.broadcasted_iota(jnp.int32, (8, LANES), 0)
        index = lax.broadcasted_iota(jnp.int32, every.shape, 0) * spans + lax.broadcasted_iota(
            jnp.int32, every.shape, 1
        )
        real = lax.broadcasted_iota(jnp.int32, every.shape, 1) < spans
        front = lane < heads
        r = chosen[0]
        table = jnp.zeros((8, LANES), F32)
        for k in range(spans):
            j = s * spans + k
            forward_on = real & (index > j) & (index <= r) & front[None]
            backward_on = real & (index < j) & (index >= r) & (~front)[None]
            total = jnp.sum(jnp.where(forward_on | backward_on, every, 0.0), axis=0)
            total = jnp.sum(total, axis=0, keepdims=True)
            ahead_on = jnp.where(j <= r, 1.0, 0.0)
            behind_on = jnp.where(j >= r, 1.0, 0.0)
            found = jnp.exp(total) * jnp.where(front, ahead_on, behind_on)
            table = jnp.where(sub == k, found, table)
        table = jnp.transpose(
            jnp.concatenate([table, jnp.zeros((LANES - 8, LANES), F32)], axis=0)
        )
        pairs = heads // 2
        dense = jnp.zeros((pairs, LANES), F32)
        for k in range(spans):
            for d in range(2):
                weight = jnp.broadcast_to(
                    table[d * heads : (d + 1) * heads, k : k + 1], (heads, LANES)
                )
                spread[d] = weight
                even = spread[d, pl.ds(0, pairs, stride=2), :]
                odd = spread[d, pl.ds(1, pairs, stride=2), :]
                dense = dense + jnp.where(low, even, odd) * reads[k, d, 0:pairs, :]
        parts[s, 0:pairs, :] = dense

        @pl.loop(1, n)
        def _(k):
            part_copy(k).start()

    def square(k):
        return pltpu.make_async_remote_copy(
            src_ref=squares.at[c],
            dst_ref=squares.at[c],
            send_sem=sem_sq.at[0],
            recv_sem=sem_sq.at[1],
            device_id={"sp": s, "tp": mate(k)},
            device_id_type=MESH,
        )

    def gather_read():
        count(parts, n - 1, sem_y.at[1]).wait()

        def add_part(i, total):
            return total + parts[i]

        total = lax.fori_loop(1, n, add_part, parts[0])[0 : heads // 2]
        spread[0, pl.ds(0, heads // 2, stride=2), :] = total
        spread[0, pl.ds(1, heads // 2, stride=2), :] = pltpu.roll(total, P_SIZE, 1)
        door = gate[0].astype(F32) * 0.5
        gated = spread[0][:, :P_SIZE] * silu_of_half(door)
        spread[1, :, 0:P_SIZE] = gated
        squares[c] = jnp.broadcast_to(jnp.sum(gated * gated, keepdims=True), (8, LANES))
        for k in range(1, width):
            square(k).start()

    def finish_read():
        count(squares, width - 1, sem_sq.at[1]).wait()
        mean = jnp.sum(squares[...], axis=0)[0:1, 0:1] / (H * P_SIZE)
        gated = spread[1, :, 0:P_SIZE]
        fr[0] = (gated * lax.rsqrt(mean + EPSILON) * gain[...]).astype(BF16)

    @pl.when(is_mid)
    def _():
        take(2, early)
        pass_on(early)

    @pl.loop(0, 3)
    def _(i):
        u = jnp.where(is_end, i, lax.rem(i + 1, 3))

        @pl.when(i > 0)
        def _():
            handed(u)

        process(u, False)

        @pl.when(i == 0)
        def _():
            @pl.when(is_end)
            def _():
                for piece in everything:
                    send_own(1, piece).start()
                take(1)
                hand_on(1)

            @pl.when(is_mid)
            def _():
                take(2, late)
                pass_on(late)
                hand_on(2)
                take(0)
                hand_on(0)

            own_read()

        @pl.when(i == 1)
        def _():
            @pl.when(is_mid)
            def _():
                take(3, early)
                hand_on(3, early)

            send_read()

            @pl.when(is_end)
            def _():
                take(2)
                hand_on(2)

            @pl.when(is_mid)
            def _():
                handed(3, early)
                process(3, True, 0)
                take(3, late)
                hand_on(3, late)
                handed(3, late)
                for k in range(1, spans):
                    process(3, True, k)

    gather_read()
    finish_read()

    @pl.when(s < n - 1)
    def _():
        edge(1).wait_send()

    @pl.when(s > 0)
    def _():
        edge(0).wait_send()

    for j in range(2):
        left(sem_x.at[j], zz).wait()
    for u in range(3):
        left(sem_hand.at[0, u, 0], u, width - 1).wait()
    count(squares, width - 1, sem_sq.at[0]).wait()
    count(logs, n - 1, sem_c.at[0]).wait()
    count(parts, n - 1, sem_y.at[0]).wait()

    @pl.when(is_mid)
    def _():
        left(sem_fwd, 2).wait()
        left(sem_hand.at[0, 3, 0], 3, width - 1).wait()
        count(out, LINE * spans, sem_self).wait()
        count(out, LINE * (ny - 1) * spans, sem_out.at[0]).wait()
        count(out, ny * spans, sem_out.at[1]).wait()
        count(out, LINE * (ny - 1) * spans, sem_out.at[2]).wait()

    @pl.when(is_end)
    def _():
        count(out, (LINE - 1) * spans, sem_self).wait()
        count(out, (LINE - 1) * (ny - 1) * spans, sem_out.at[0]).wait()
        count(out, ((LINE - 1) * (ny - 1) + ny) * spans, sem_out.at[2]).wait()


def per_device(x, xw, bw, dtw, bias, rate, cx, cb, q, gate, chosen, gain):
    n = lax.axis_size("sp")
    width = lax.axis_size("tp")
    tokens, feats = x.shape
    depth = xw.shape[0]
    spans = tokens // SPAN
    heads = xw.shape[1] // P_SIZE
    groups = heads // PER
    blocks = heads // TILE
    columns = N * P_SIZE // n
    ny = n // LINE
    share = N // LINE
    gb = min(PER, groups)
    kblocks = groups // gb
    kcols = kblocks * LANES
    pblocks = TILE * P_SIZE // LANES
    tall = tokens + EDGE + 8
    small = (bias, rate, cx, cb, q, gate, gain)
    anywhere = pl.BlockSpec(memory_space=pl.ANY)
    vmem = pl.BlockSpec(memory_space=pltpu.VMEM)
    dma = pltpu.SemaphoreType.DMA
    return pl.pallas_call(
        functools.partial(kernel, n, width),
        out_shape=(
            pltpu.VMEM((spans * n, 2, heads, columns), BF16),
            pltpu.VMEM((1, heads, P_SIZE), BF16),
        ),
        in_specs=[anywhere] * 10 + [pl.BlockSpec(memory_space=pltpu.SMEM), anywhere],
        out_specs=(vmem, vmem),
        scratch_shapes=[pltpu.VMEM(a.shape, a.dtype) for a in small]
        + [
            pltpu.VMEM((LINE, tokens + EDGE, depth), BF16),
            pltpu.VMEM(xw.shape, BF16),
            pltpu.VMEM(bw.shape, BF16),
            pltpu.VMEM((depth, kcols + 2 * H), BF16),
            pltpu.VMEM((depth, kcols), BF16),
            pltpu.VMEM((pblocks, tall, LANES), F32),
            pltpu.VMEM((pblocks, tall, LANES), F32),
            pltpu.VMEM((kblocks + 1, tall, LANES), F32),
            pltpu.VMEM((tokens, heads * P_SIZE), BF16),
            pltpu.VMEM((spans, kcols, LANES), F32),
            pltpu.VMEM((spans, kcols, LANES), F32),
            pltpu.VMEM((spans, 2 * heads, LANES), F32),
            pltpu.VMEM((2, TILE * (share + 4) + share, LANES), F32),
            pltpu.VMEM((LINE + 1, spans, ny, blocks, 2, TILE, columns), BF16),
            pltpu.VMEM((8, cx.shape[1]), F32),
            pltpu.VMEM((8, cb.shape[1]), F32),
            pltpu.VMEM((8, kcols), F32),
            pltpu.VMEM((8, kcols), F32),
            pltpu.VMEM((2 * SPAN, 2 * SPAN), BF16),
            pltpu.VMEM((2, LANES, LANES), F32),
            pltpu.VMEM((2 * heads, LANES), F32),
            pltpu.VMEM((2 * heads, LANES), F32),
            pltpu.VMEM((8, N), F32),
            pltpu.VMEM((2, heads, LANES), F32),
            pltpu.VMEM((n, 8, LANES), F32),
            pltpu.VMEM((n, max(8, heads // 2), LANES), F32),
            pltpu.VMEM((max(8, heads // 2), LANES), F32),
            pltpu.VMEM((spans, 2, max(8, heads // 2), LANES), F32),
            pltpu.VMEM((width, 8, LANES), F32),
            dma((8,)),
            dma((2,)),
            dma,
            dma((2, 2)),
            dma((2,)),
            dma((LINE, 2)),
            dma,
            dma((2, LINE, 2)),
            dma((2,)),
            dma((2,)),
            dma((2,)),
            dma((3,)),
            dma,
            pltpu.SemaphoreType.REGULAR((3,)),
        ],
        compiler_params=pltpu.CompilerParams(
            collective_id=0, has_side_effects=True, vmem_limit_bytes=56 * 1024 * 1024
        ),
    )(x, xw, bw, dtw, bias, rate, cx, cb, q, gate, chosen, gain)


def solution(mesh):
    return jax.shard_map(
        per_device,
        mesh=mesh,
        in_specs=(
            P(("gr", "sp"), "tp"),
            P(None, "tp"),
            P(None, "tp"),
            P(),
            P(),
            P(),
            P(None, "tp"),
            P(None, "tp"),
            P("gr", "tp", None),
            P("gr", "tp", None),
            P("gr"),
            P("tp", None),
        ),
        out_specs=(P("gr", None, "tp", "sp"), P("gr", "tp", None)),
        check_vma=False,
    )
```
